32 devices in a mesh: sp: 16 (over z, y, x), tp: 2 (over core).
Axes of the slice: x: 2, y: 2, z: 4, core: 2. Of those that a mesh axis runs over, the one named last changes fastest.
Arguments:
- tokens: bfloat16 [4096, 2048], P(('sp', 'tp')), may hold values from -6 to 6
- mix_gain: float32 [2048], replicated, may hold values from 0.1 to 1.9
- query_proj: bfloat16 [2048, 1536], P(None, 'tp'), may hold values from -4 to 4
- compressed_projection: bfloat16 [2048, 256], replicated, may hold values from -0.125 to 0.125
- compressed_norm_gain: float32 [256], replicated, may hold values from 0.1 to 1.9
- rope_proj: bfloat16 [2048, 64], replicated, may hold values from -0.125 to 0.125
- key_up: bfloat16 [256, 1024], P(None, 'tp'), may hold values from -4 to 4
- value_up_weight: bfloat16 [256, 1024], P(None, 'tp'), may hold values from -0.375 to 0.375
- scan_input: bfloat16 [2048, 2048], P('sp', 'tp'), may hold values from -0.125 to 0.125
- scan_gate: bfloat16 [2048, 2048], P('sp', 'tp'), may hold values from -0.125 to 0.125
- scan_write: bfloat16 [2048, 1024], P('sp', 'tp'), may hold values from -0.125 to 0.125
- scan_read: bfloat16 [2048, 1024], P('sp', 'tp'), may hold values from -0.125 to 0.125
- step_proj: bfloat16 [2048, 32], replicated, may hold values from -0.125 to 0.125
- conv_input: bfloat16 [4, 2048], P(None, 'tp'), may hold values from -3 to 3
- conv_write: bfloat16 [4, 1024], P(None, 'tp'), may hold values from -3 to 3
- conv_read: bfloat16 [4, 1024], P(None, 'tp'), may hold values from -3 to 3
- decay_log: float32 [32], P('tp'), may hold values from -16 to -2.8
- decay_offset: float32 [4096, 32], P('sp', 'tp'), may hold values from -2.2 to 0
- skip_gain: float32 [32], P('tp'), may hold values from 0.1 to 1.9
- group_gain: float32 [2048], P('tp'), may hold values from 0.1 to 1.9
Outputs:
- attended: bfloat16 [4096, 1024], P('sp', 'tp')
- scanned: bfloat16 [4096, 2048], P('sp', 'tp')
The draws below stay inside these ranges and needn't reach their ends.
All inputs are finite; a program needn't handle non-finite values.
Results may differ from the reference program's by a relative error of at most 0.017.
The reference program's roundings to bfloat16 on the way count: a program that leaves them out, or rounds other values in their place, can miss the bound.
Values may be sent and summed in bfloat16 or wider, within the bound.
A program may use at most 128 MiB of HBM per device.

```python
import jax
import jax.numpy as jnp
from jax import lax

MODEL_WIDTH = 2048
ATTENTION_HEADS = 8
UNROTATED_WIDTH = 128
ROPE = 64
VALUE_WIDTH = 128
LATENT_KEY_WIDTH = 256
SSM_HEADS = 32
SSM_DIM = 64
SSM_GROUPS = 8
SSM_STATE = 128
CONV = 4
BLOCK = 128
TOK_DEV = 256
SEQ = 4096


def draw_decay_log(key, part):
    pick_key, fast_key, slow_key = jax.random.split(jax.random.fold_in(key, 11), 3)
    fast = jax.random.uniform(pick_key, (SSM_HEADS,), jnp.float32) < 0.5
    fast_rate = jnp.exp(jax.random.uniform(fast_key, (SSM_HEADS,), jnp.float32, jnp.log(0.02), jnp.log(0.06)))
    slow_rate = jnp.exp(jax.random.uniform(slow_key, (SSM_HEADS,), jnp.float32, jnp.log(0.05), jnp.log(0.3))) / SEQ
    return jnp.log(jnp.where(fast, fast_rate, slow_rate)).astype(jnp.float32)


def draw_decay_offset(key, part):
    rate_key, place_key, depth_key = jax.random.split(jax.random.fold_in(key, 23), 3)
    blocks = SEQ // TOK_DEV
    rates = jnp.exp(jax.random.uniform(rate_key, (blocks, SSM_HEADS), jnp.float32, jnp.log(0.1), jnp.log(0.6)))
    reference_amount = -jnp.repeat(rates, TOK_DEV, axis=0) / SEQ
    places = jax.random.randint(place_key, (3,), 0, SEQ)
    layer_tiers = jnp.log(jax.random.uniform(depth_key, (3,), jnp.float32, 0.5, 0.8))
    match_flags = (jnp.arange(SEQ)[:, None] == places[None, :]).astype(jnp.float32)
    sudden_outlier = jnp.dot(match_flags, layer_tiers)[:, None]
    return (reference_amount + sudden_outlier).astype(jnp.float32)


def shared_direction(key):
    order_key, strength_key, direction_key = jax.random.split(jax.random.fold_in(key, 37), 3)
    chosen = (jax.random.permutation(order_key, ATTENTION_HEADS) < ATTENTION_HEADS // 2).astype(jnp.float32)
    strength = jnp.exp(jax.random.uniform(strength_key, (ATTENTION_HEADS,), jnp.float32, jnp.log(6.0), jnp.log(18.0)))
    direction = jax.random.normal(direction_key, (ATTENTION_HEADS, UNROTATED_WIDTH), jnp.float32)
    direction = direction / jnp.sqrt(jnp.sum(direction * direction, axis=1, keepdims=True))
    magnitude = jnp.sqrt(strength * jnp.sqrt(jnp.float32(UNROTATED_WIDTH + ROPE)))
    return direction * (magnitude * chosen)[:, None]


def draw_query_proj(key, part):
    planted = shared_direction(key)
    noise_random_key, along_sequence_key = jax.random.split(jax.random.fold_in(key, 41))
    reference_amount = jnp.clip(jax.random.normal(noise_random_key, (MODEL_WIDTH, ATTENTION_HEADS * (UNROTATED_WIDTH + ROPE)), jnp.float32), -6.0, 6.0) / jnp.sqrt(jnp.float32(MODEL_WIDTH))
    along_sequence = jax.random.normal(along_sequence_key, (MODEL_WIDTH,), jnp.float32)
    along_sequence = along_sequence / jnp.sqrt(jnp.sum(along_sequence * along_sequence))
    padded = jnp.concatenate([planted, jnp.zeros((ATTENTION_HEADS, ROPE), jnp.float32)], axis=1).reshape(ATTENTION_HEADS * (UNROTATED_WIDTH + ROPE))
    return jnp.clip(reference_amount + along_sequence[:, None] * padded[None, :], -4.0, 4.0).astype(jnp.bfloat16)


def draw_key_up(key, part):
    planted = shared_direction(key)
    noise_random_key, along_sequence_key = jax.random.split(jax.random.fold_in(key, 43))
    reference_amount = jnp.clip(jax.random.normal(noise_random_key, (LATENT_KEY_WIDTH, ATTENTION_HEADS * UNROTATED_WIDTH), jnp.float32), -6.0, 6.0) / jnp.sqrt(jnp.float32(LATENT_KEY_WIDTH))
    along_sequence = jax.random.normal(along_sequence_key, (LATENT_KEY_WIDTH,), jnp.float32)
    along_sequence = along_sequence / jnp.sqrt(jnp.sum(along_sequence * along_sequence))
    flat = planted.reshape(ATTENTION_HEADS * UNROTATED_WIDTH)
    return jnp.clip(reference_amount + along_sequence[:, None] * flat[None, :], -4.0, 4.0).astype(jnp.bfloat16)


def levels(own_key, shape, cuts, low, top_value):
    def one(dim, shards_of):
        draws = jax.random.uniform(jax.random.fold_in(jax.random.fold_in(own_key, 6), dim), (shards_of,), jnp.float32, low / len(cuts), top_value / len(cuts))
        return jnp.repeat(jnp.exp(draws), shape[dim] // shards_of).reshape((-1,) + (1,) * (len(shape) - dim - 1))

    level = one(*cuts[0])
    for cut in cuts[1:]:
        level = level * one(*cut)
    return level


def gaussian(own_key, extent, deviation, bound, shards=(), kind=jnp.bfloat16):
    drawn = jax.random.normal(own_key, extent, jnp.float32) * deviation
    if len(shards) > 0:
        drawn = levels(own_key, extent, shards, -0.22, 0.18) * drawn
    return jnp.clip(drawn, min=-bound, max=bound).astype(kind)


def setup_inputs(seed: int = 0) -> dict:
    seeds = jax.random.split(jax.random.key(seed), 21)
    return {
        "tokens": gaussian(seeds[0], (SEQ, MODEL_WIDTH), 1.0, 6.0, ((0, 32),)),
        "mix_gain": jnp.clip(1.0 + 0.18 * jax.random.normal(seeds[1], (MODEL_WIDTH,), jnp.float32), 0.1, 1.9),
        "query_proj": draw_query_proj(jax.random.fold_in(seeds[20], 71), 0),
        "compressed_projection": gaussian(seeds[3], (MODEL_WIDTH, LATENT_KEY_WIDTH), MODEL_WIDTH ** -0.5, 0.125),
        "compressed_norm_gain": jnp.clip(1.0 + 0.18 * jax.random.normal(seeds[4], (LATENT_KEY_WIDTH,), jnp.float32), 0.1, 1.9),
        "rope_proj": gaussian(seeds[5], (MODEL_WIDTH, ROPE), MODEL_WIDTH ** -0.5, 0.125),
        "key_up": draw_key_up(jax.random.fold_in(seeds[20], 71), 0),
        "value_up_weight": gaussian(seeds[7], (LATENT_KEY_WIDTH, ATTENTION_HEADS * VALUE_WIDTH), LATENT_KEY_WIDTH ** -0.5, 0.375, ((1, 2),)),
        "scan_input": gaussian(seeds[8], (MODEL_WIDTH, SSM_HEADS * SSM_DIM), MODEL_WIDTH ** -0.5, 0.125, ((0, 16), (1, 2))),
        "scan_gate": gaussian(seeds[9], (MODEL_WIDTH, SSM_HEADS * SSM_DIM), MODEL_WIDTH ** -0.5, 0.125, ((0, 16), (1, 2))),
        "scan_write": gaussian(seeds[10], (MODEL_WIDTH, SSM_GROUPS * SSM_STATE), MODEL_WIDTH ** -0.5, 0.125, ((0, 16), (1, 2))),
        "scan_read": gaussian(seeds[11], (MODEL_WIDTH, SSM_GROUPS * SSM_STATE), MODEL_WIDTH ** -0.5, 0.125, ((0, 16), (1, 2))),
        "step_proj": gaussian(seeds[12], (MODEL_WIDTH, SSM_HEADS), MODEL_WIDTH ** -0.5, 0.125),
        "conv_input": gaussian(seeds[13], (CONV, SSM_HEADS * SSM_DIM), CONV ** -0.5, 3.0, ((1, 2),)),
        "conv_write": gaussian(seeds[14], (CONV, SSM_GROUPS * SSM_STATE), CONV ** -0.5, 3.0, ((1, 2),)),
        "conv_read": gaussian(seeds[15], (CONV, SSM_GROUPS * SSM_STATE), CONV ** -0.5, 3.0, ((1, 2),)),
        "decay_log": draw_decay_log(jax.random.fold_in(seeds[20], 71), 0),
        "decay_offset": draw_decay_offset(jax.random.fold_in(seeds[20], 71), 0),
        "skip_gain": jnp.clip(1.0 + 0.18 * jax.random.normal(seeds[18], (SSM_HEADS,), jnp.float32), 0.1, 1.9),
        "group_gain": jnp.clip(1.0 + 0.18 * jax.random.normal(seeds[19], (SSM_HEADS * SSM_DIM,), jnp.float32), 0.1, 1.9),
    }


eps = 1e-06
theta = 10000.0
floor_score = -1e+30

def rms_scale(values, gain):
    wide = values.astype(jnp.float32)
    return wide * lax.rsqrt(lax.optimization_barrier(jnp.mean(wide * wide, axis=-1, keepdims=True)) + eps) * gain

def rotate(values, positions):
    half = values.shape[-1] // 2
    freqs = theta ** (-jnp.arange(half, dtype=jnp.float32) * 2.0 / values.shape[-1])
    angle = positions.astype(jnp.float32)[:, None] * freqs[None, :]
    cosine = jnp.cos(angle)
    sine = jnp.sin(angle)
    if values.ndim == 3:
        cosine = cosine[:, None, :]
        sine = sine[:, None, :]
    first = values[..., :half]
    second = values[..., half:]
    return jnp.concatenate([first * cosine - second * sine, second * cosine + first * sine], axis=-1)

def short_conv(values, edge, taps):
    span = taps.shape[0]
    length = values.shape[0]
    padded = jnp.concatenate([edge, values], axis=0).astype(jnp.float32)
    result = jnp.zeros(values.shape, jnp.float32)
    for index in range(span):
        result = result + taps[index].astype(jnp.float32)[None, :] * padded[index:index + length]
    return jax.nn.silu(result).astype(jnp.bfloat16)

def blockwise_scan(heads, steps, decays, writes, reads, state, block):
    count = heads.shape[0] // block
    best = lax.Precision.HIGHEST

    def split(values):
        return values.reshape((count, block) + values.shape[1:])

    def one_block(state, inputs):
        head_block, step_block, decay_block, write_block, read_block = inputs
        running = jnp.cumsum(decay_block, axis=0)
        causal = jnp.tril(jnp.ones((block, block), dtype=bool))[:, :, None, None]
        spread = running[:, None] - running[None, :]
        fading = jnp.where(causal, jnp.exp(jnp.where(causal, spread, 0.0)), 0.0)
        inner = jnp.einsum('lgn,sgn->lsg', read_block, write_block, precision=best)
        mixing = inner[..., None] * fading * step_block[None]
        within = jnp.einsum('lsgr,sgrp->lgrp', mixing, head_block, precision=best)
        carried = jnp.einsum('lgn,grpn->lgrp', read_block, state, precision=best) * jnp.exp(running)[..., None]
        to_end = jnp.exp(running[-1:] - running) * step_block
        update = jnp.einsum('sgn,sgr,sgrp->grpn', write_block, to_end, head_block, precision=best)
        state = jnp.exp(running[-1])[..., None, None] * state + update
        return (state, within + carried)
    state, outputs = lax.scan(one_block, state, (split(heads), split(steps), split(decays), split(writes), split(reads)))
    return (state, outputs.reshape(heads.shape))

def gated_norm(mixed, gate, gain):
    length = mixed.shape[0]
    groups = mixed.shape[1]
    flat = mixed.reshape(length, groups, -1)
    gated = flat * jax.nn.silu(gate.astype(jnp.float32)).reshape(length, groups, -1)
    scaled = gated * lax.rsqrt(lax.optimization_barrier(jnp.mean(gated * gated, axis=-1, keepdims=True)) + eps)
    return (scaled * gain.reshape(groups, -1)[None]).reshape(length, -1).astype(jnp.bfloat16)

def reference(tokens, mix_gain, query_proj, compressed_projection, compressed_norm_gain, rope_proj, key_up, value_up_weight, scan_input, scan_gate, scan_write, scan_read, step_proj, conv_input, conv_write, conv_read, decay_log, decay_offset, skip_gain, group_gain):
    positions = jnp.arange(SEQ, dtype=jnp.int32)
    normed = rms_scale(tokens, mix_gain).astype(jnp.bfloat16)
    query = jnp.dot(normed, query_proj, preferred_element_type=jnp.float32).astype(jnp.bfloat16)
    query = query.reshape(SEQ, ATTENTION_HEADS, UNROTATED_WIDTH + ROPE)
    query_plain = query[:, :, :UNROTATED_WIDTH]
    query_turned = rotate(query[:, :, UNROTATED_WIDTH:].astype(jnp.float32), positions).astype(jnp.bfloat16)
    latent = rms_scale(jnp.dot(normed, compressed_projection, preferred_element_type=jnp.float32), compressed_norm_gain).astype(jnp.bfloat16)
    key_turned = rotate(jnp.dot(normed, rope_proj, preferred_element_type=jnp.float32), positions).astype(jnp.bfloat16)
    key_plain = jnp.dot(latent, key_up, preferred_element_type=jnp.float32).astype(jnp.bfloat16).reshape(SEQ, ATTENTION_HEADS, UNROTATED_WIDTH)
    values = jnp.dot(latent, value_up_weight, preferred_element_type=jnp.float32).astype(jnp.bfloat16).reshape(SEQ, ATTENTION_HEADS, VALUE_WIDTH)
    scale = (UNROTATED_WIDTH + ROPE) ** (-0.5)

    def one_query_block(index):
        start = index * TOK_DEV
        q_plain = lax.dynamic_slice_in_dim(query_plain, start, TOK_DEV, 0).astype(jnp.float32)
        q_turned = lax.dynamic_slice_in_dim(query_turned, start, TOK_DEV, 0).astype(jnp.float32)
        q_positions = start + jnp.arange(TOK_DEV, dtype=jnp.int32)

        def visit(step, carry):
            highest, total, summed = carry
            k_start = step * TOK_DEV
            k_plain = lax.dynamic_slice_in_dim(key_plain, k_start, TOK_DEV, 0).astype(jnp.float32)
            k_turned = lax.dynamic_slice_in_dim(key_turned, k_start, TOK_DEV, 0).astype(jnp.float32)
            k_values = lax.dynamic_slice_in_dim(values, k_start, TOK_DEV, 0).astype(jnp.float32)
            k_positions = k_start + jnp.arange(TOK_DEV, dtype=jnp.int32)
            scores = jnp.einsum('qhd,khd->hqk', q_plain, k_plain) + jnp.einsum('qhd,kd->hqk', q_turned, k_turned)
            scores = scores * scale
            scores = jnp.where(k_positions[None, None, :] <= q_positions[None, :, None], scores, -jnp.inf)
            new_highest = jnp.maximum(highest, lax.optimization_barrier(jnp.max(scores, axis=-1)))
            weights = jnp.exp(scores - new_highest[..., None])
            shrink = jnp.exp(highest - new_highest)
            total = total * shrink + lax.optimization_barrier(jnp.sum(weights, axis=-1))
            rounded = lax.optimization_barrier(weights.astype(jnp.bfloat16)).astype(jnp.float32)
            summed = summed * shrink[..., None] + jnp.einsum('hqk,khd->hqd', rounded, k_values)
            return (new_highest, total, summed)
        initial_recurrent = (jnp.full((ATTENTION_HEADS, TOK_DEV), floor_score, jnp.float32), jnp.zeros((ATTENTION_HEADS, TOK_DEV), jnp.float32), jnp.zeros((ATTENTION_HEADS, TOK_DEV, VALUE_WIDTH), jnp.float32))
        highest, total, summed = lax.fori_loop(0, index + 1, visit, initial_recurrent)
        return (summed / total[..., None]).astype(jnp.bfloat16)
    blocks = lax.map(one_query_block, jnp.arange(SEQ // TOK_DEV, dtype=jnp.int32))
    attended = jnp.transpose(blocks, (0, 2, 1, 3)).reshape(SEQ, ATTENTION_HEADS * VALUE_WIDTH)
    groups = SSM_GROUPS
    per_group = SSM_HEADS // SSM_GROUPS
    head_raw = jnp.dot(normed, scan_input, preferred_element_type=jnp.float32).astype(jnp.bfloat16)
    gate = jnp.dot(normed, scan_gate, preferred_element_type=jnp.float32).astype(jnp.bfloat16)
    write_raw = jnp.dot(normed, scan_write, preferred_element_type=jnp.float32).astype(jnp.bfloat16)
    read_raw = jnp.dot(normed, scan_read, preferred_element_type=jnp.float32).astype(jnp.bfloat16)
    step_size = jax.nn.softplus(jnp.dot(normed, step_proj, preferred_element_type=jnp.float32))
    heads = short_conv(head_raw, jnp.zeros((CONV - 1, head_raw.shape[1]), jnp.bfloat16), conv_input)
    writes = short_conv(write_raw, jnp.zeros((CONV - 1, write_raw.shape[1]), jnp.bfloat16), conv_write)
    reads = short_conv(read_raw, jnp.zeros((CONV - 1, read_raw.shape[1]), jnp.bfloat16), conv_read)
    log_decay = -jnp.exp(decay_log)[None, :] * step_size + decay_offset
    head_values = heads.astype(jnp.float32).reshape(SEQ, groups, per_group, SSM_DIM)
    step_values = step_size.reshape(SEQ, groups, per_group)
    decay_values = log_decay.reshape(SEQ, groups, per_group)
    write_values = writes.astype(jnp.float32).reshape(SEQ, groups, SSM_STATE)
    output_entries = reads.astype(jnp.float32).reshape(SEQ, groups, SSM_STATE)
    empty_state = jnp.zeros((groups, per_group, SSM_DIM, SSM_STATE), jnp.float32)
    final_state, mixed = blockwise_scan(head_values, step_values, decay_values, write_values, output_entries, empty_state, BLOCK)
    mixed = mixed + skip_gain.reshape(groups, per_group)[None, :, :, None] * head_values
    scanned = gated_norm(mixed, gate, group_gain)
    return (attended, scanned)
```

```python
import jax
import jax.numpy as jnp
from jax import lax
from jax.sharding import PartitionSpec as P

UNROTATED_WIDTH = 128
ROPE = 64
VALUE_WIDTH = 128
SSM_DIM = 64
SSM_STATE = 128


eps = 1e-06
theta = 10000.0
floor_score = -1e30


def from_behind(value, axis, steps):
    count = lax.axis_size(axis)
    initial, last = (max(0, -steps), min(count, count - steps))
    return lax.ppermute(value, axis, [(source, source + steps) for source in range(initial, last)])


def rms_scale(values, gain):
    wide = values.astype(jnp.float32)
    return wide * lax.rsqrt(jnp.mean(wide * wide, axis=-1, keepdims=True) + eps) * gain


def rotate(values, positions):
    half = values.shape[-1] // 2
    freqs = theta ** (-jnp.arange(half, dtype=jnp.float32) * 2.0 / values.shape[-1])
    angle = positions.astype(jnp.float32)[:, None] * freqs[None, :]
    cosine = jnp.cos(angle)
    sine = jnp.sin(angle)
    if values.ndim == 3:
        cosine = cosine[:, None, :]
        sine = sine[:, None, :]
    first = values[..., :half]
    second = values[..., half:]
    return jnp.concatenate(
        [first * cosine - second * sine, second * cosine + first * sine], axis=-1
    )


def short_conv(values, edge, taps):
    span = taps.shape[0]
    length = values.shape[0]
    padded = jnp.concatenate([edge, values], axis=0).astype(jnp.float32)
    result = jnp.zeros(values.shape, jnp.float32)
    for index in range(span):
        result = result + taps[index].astype(jnp.float32)[None, :] * padded[index : index + length]
    return jax.nn.silu(result).astype(jnp.bfloat16)


def local_scan(heads, steps, decays, writes, reads):
    length = decays.shape[-1]
    running = jnp.einsum(
        "grs,ls->grl",
        decays,
        jnp.tril(jnp.ones((length, length), jnp.float32)),
        precision=lax.Precision.HIGHEST,
    )
    causal = jnp.tril(jnp.ones((length, length), dtype=bool))
    spread = jnp.where(causal, running[..., :, None] - running[..., None, :], -jnp.inf)
    inner = jnp.einsum("gln,gsn->gls", reads, writes, preferred_element_type=jnp.float32)
    mixing = inner[:, None] * jnp.exp(spread) * steps[:, :, None, :]
    within = jnp.einsum(
        "grls,grsp->grlp",
        mixing.astype(jnp.bfloat16),
        heads,
        preferred_element_type=jnp.float32,
    )
    to_end = jnp.exp(running[..., -1:] - running) * steps
    weighted = (heads.astype(jnp.float32) * to_end[..., None]).astype(jnp.bfloat16)
    state = jnp.einsum(
        "grsp,gsn->grpn", weighted, writes, preferred_element_type=jnp.float32
    )
    return running, state, within


def state_before(state, total, axis):
    groups, per_group, dim, entries = state.shape
    count = groups * per_group
    flat = state.reshape(count * dim, entries).astype(jnp.bfloat16)
    high = total.reshape(count).astype(jnp.bfloat16)
    low = (total.reshape(count) - high.astype(jnp.float32)).astype(jnp.bfloat16)
    tail = jnp.zeros((16, entries), jnp.bfloat16)
    tail = tail.at[0, :count].set(high).at[1, :count].set(low)
    everything = lax.all_gather(jnp.concatenate([flat, tail], axis=0), axis)
    here = lax.axis_index(axis)
    devices = everything.shape[0]
    states = everything[:, : count * dim].reshape(devices, count, dim, entries)
    totals = everything[:, count * dim, :count].astype(jnp.float32) + everything[
        :, count * dim + 1, :count
    ].astype(jnp.float32)
    index = jnp.arange(devices)
    between = (index[None, :] > index[:, None]) & (index[None, :] < here)
    path = jnp.sum(jnp.where(between[:, :, None], totals[None], 0.0), axis=1)
    factor = jnp.where((index < here)[:, None], jnp.exp(path), 0.0)
    before = jnp.sum(states.astype(jnp.float32) * factor[:, :, None, None], axis=0)
    return before.reshape(state.shape)


def gated_norm(mixed, gate, gain):
    length = mixed.shape[0]
    groups = mixed.shape[1]
    flat = mixed.reshape(length, groups, -1)
    gated = flat * jax.nn.silu(gate.astype(jnp.float32)).reshape(length, groups, -1)
    scaled = gated * lax.rsqrt(jnp.mean(gated * gated, axis=-1, keepdims=True) + eps)
    return (scaled * gain.reshape(groups, -1)[None]).reshape(length, -1).astype(jnp.bfloat16)


def attend_piece(
    carry,
    query_plain,
    query_turned,
    query_positions,
    latent,
    key_turned,
    key_positions,
    key_up,
    value_up_weight,
):
    highest, total, summed = carry
    heads = query_plain.shape[1]
    count = latent.shape[0]
    key_plain = (
        jnp.dot(latent, key_up, preferred_element_type=jnp.float32)
        .astype(jnp.bfloat16)
        .reshape(count, heads, -1)
    )
    values = (
        jnp.dot(latent, value_up_weight, preferred_element_type=jnp.float32)
        .astype(jnp.bfloat16)
        .reshape(count, heads, -1)
    )
    scale = (query_plain.shape[-1] + query_turned.shape[-1]) ** (-0.5)
    query_whole = jnp.concatenate([query_plain, query_turned], axis=-1)
    shared_turned = jnp.broadcast_to(key_turned[:, None, :], (count, heads, key_turned.shape[-1]))
    key_whole = jnp.concatenate([key_plain, shared_turned], axis=-1)
    scores = (
        jnp.einsum("qhd,khd->hqk", query_whole, key_whole, preferred_element_type=jnp.float32)
        * scale
    )
    scores = jnp.where(
        key_positions[None, None, :] <= query_positions[None, :, None], scores, -jnp.inf
    )
    new_highest = jnp.maximum(highest, jnp.max(scores, axis=-1))
    weights = jnp.exp(scores - new_highest[..., None])
    total = jnp.sum(weights, axis=-1)
    summed = jnp.einsum(
        "hqk,khd->hqd", weights.astype(jnp.bfloat16), values, preferred_element_type=jnp.float32
    )
    return (new_highest, total, summed)


def shards(
    tokens,
    mix_gain,
    query_proj,
    compressed_projection,
    compressed_norm_gain,
    rope_proj,
    key_up,
    value_up_weight,
    scan_input,
    scan_gate,
    scan_write,
    scan_read,
    step_proj,
    conv_input,
    conv_write,
    conv_read,
    decay_log,
    decay_offset,
    skip_gain,
    group_gain,
):
    own_normed = rms_scale(tokens, mix_gain).astype(jnp.bfloat16)
    rows = lax.all_gather(own_normed, "tp", axis=0, tiled=True)
    length = rows.shape[0]
    width = tokens.shape[1]
    sp_index = lax.axis_index("sp")
    positions = sp_index * length + jnp.arange(length, dtype=jnp.int32)
    heads = key_up.shape[1] // UNROTATED_WIDTH
    local_heads = decay_log.shape[0]
    latent_width = compressed_projection.shape[1]
    small = jnp.dot(
        rows,
        jnp.concatenate([compressed_projection, rope_proj, step_proj], axis=1),
        preferred_element_type=jnp.float32,
    )
    latent = rms_scale(small[:, :latent_width], compressed_norm_gain).astype(jnp.bfloat16)
    key_turned = rotate(small[:, latent_width : latent_width + ROPE], positions).astype(
        jnp.bfloat16
    )
    step_all = small[:, latent_width + ROPE :]
    edge_rows = from_behind(rows[length - 8 :], "sp", 1)
    keys = jnp.concatenate([latent, key_turned], axis=1)
    depth = scan_input.shape[0]
    packed = jnp.concatenate(
        [scan_input, scan_gate, scan_write, scan_read, keys.reshape(depth, -1)], axis=1
    )
    everything = lax.all_gather(packed, "sp", axis=0, tiled=True)
    widths = [w.shape[1] for w in (scan_input, scan_gate, scan_write, scan_read)]
    scan_width = sum(widths)
    all_keys = everything[:, scan_width:].reshape(-1, latent_width + ROPE)
    projected = jnp.dot(
        jnp.concatenate([edge_rows, rows], axis=0),
        everything[:, :scan_width],
        preferred_element_type=jnp.float32,
    ).astype(jnp.bfloat16)
    edge, projected = projected[:8], projected[8:]
    gate = projected[:, widths[0] : widths[0] + widths[1]]
    span = conv_input.shape[0] - 1

    def convolved(start, size, taps):
        return short_conv(
            projected[:, start : start + size], edge[8 - span :, start : start + size], taps
        )

    head_conv = convolved(0, widths[0], conv_input)
    writes = convolved(widths[0] + widths[1], widths[2], conv_write)
    reads = convolved(widths[0] + widths[1] + widths[2], widths[3], conv_read)
    step_size = jax.nn.softplus(
        lax.dynamic_slice_in_dim(step_all, lax.axis_index("tp") * local_heads, local_heads, 1)
    )
    groups = scan_write.shape[1] // SSM_STATE
    per_group = local_heads // groups
    log_decay = -jnp.exp(decay_log)[None, :] * step_size + decay_offset
    head_values = jnp.transpose(
        head_conv.reshape(length, groups, per_group, SSM_DIM), (1, 2, 0, 3)
    )
    step_values = step_size.T.reshape(groups, per_group, length)
    decay_values = log_decay.T.reshape(groups, per_group, length)
    write_values = jnp.transpose(writes.reshape(length, groups, SSM_STATE), (1, 0, 2))
    read_values = jnp.transpose(reads.reshape(length, groups, SSM_STATE), (1, 0, 2))
    running, final_state, mixed = local_scan(
        head_values, step_values, decay_values, write_values, read_values
    )
    incoming = state_before(final_state, running[..., -1], "sp")
    carried = jnp.einsum(
        "gln,grpn->grlp",
        read_values,
        incoming.astype(jnp.bfloat16),
        preferred_element_type=jnp.float32,
    )
    mixed = (
        mixed
        + carried * jnp.exp(running)[..., None]
        + skip_gain.reshape(groups, per_group)[:, :, None, None] * head_values.astype(jnp.float32)
    )
    scanned = gated_norm(jnp.transpose(mixed, (2, 0, 1, 3)), gate, group_gain)

    query = jnp.dot(rows, query_proj, preferred_element_type=jnp.float32).astype(jnp.bfloat16)
    query = query.reshape(length, heads, UNROTATED_WIDTH + ROPE)
    query_plain = query[:, :, :UNROTATED_WIDTH]
    query_turned = rotate(query[:, :, UNROTATED_WIDTH:].astype(jnp.float32), positions).astype(
        jnp.bfloat16
    )
    initial = (
        jnp.full((heads, length), floor_score, jnp.float32),
        jnp.zeros((heads, length), jnp.float32),
        jnp.zeros((heads, length, VALUE_WIDTH), jnp.float32),
    )
    key_positions = jnp.arange(all_keys.shape[0], dtype=jnp.int32)
    _, total, summed = attend_piece(
        initial,
        query_plain,
        query_turned,
        positions,
        all_keys[:, :latent_width],
        all_keys[:, latent_width:],
        key_positions,
        key_up,
        value_up_weight,
    )
    attended = jnp.transpose((summed / total[..., None]).astype(jnp.bfloat16), (1, 0, 2)).reshape(
        length, heads * VALUE_WIDTH
    )
    return (attended, scanned)


def solution(mesh):
    in_specs = (
        P(("sp", "tp"), None),
        P(),
        P(None, "tp"),
        P(),
        P(),
        P(),
        P(None, "tp"),
        P(None, "tp"),
        P("sp", "tp"),
        P("sp", "tp"),
        P("sp", "tp"),
        P("sp", "tp"),
        P(),
        P(None, "tp"),
        P(None, "tp"),
        P(None, "tp"),
        P("tp"),
        P("sp", "tp"),
        P("tp"),
        P("tp"),
    )
    out_specs = (P("sp", "tp"), P("sp", "tp"))
    return jax.shard_map(shards, mesh=mesh, in_specs=in_specs, out_specs=out_specs, check_vma=False)
```

```python
import jax
import jax.numpy as jnp
from jax import lax
from jax.experimental import pallas as pl
from jax.experimental.pallas import tpu as pltpu
from jax.sharding import PartitionSpec as P

UNROTATED_WIDTH = 128
ROPE = 64
VALUE_WIDTH = 128
SSM_DIM = 64
SSM_STATE = 128


eps = 1e-06
theta = 10000.0
floor_score = -1e30


def from_behind(value, axis, steps):
    count = lax.axis_size(axis)
    initial, last = (max(0, -steps), min(count, count - steps))
    return lax.ppermute(value, axis, [(source, source + steps) for source in range(initial, last)])


def rms_scale(values, gain):
    wide = values.astype(jnp.float32)
    return wide * lax.rsqrt(jnp.mean(wide * wide, axis=-1, keepdims=True) + eps) * gain


def rotate(values, positions):
    half = values.shape[-1] // 2
    freqs = theta ** (-jnp.arange(half, dtype=jnp.float32) * 2.0 / values.shape[-1])
    angle = positions.astype(jnp.float32)[:, None] * freqs[None, :]
    cosine = jnp.cos(angle)
    sine = jnp.sin(angle)
    if values.ndim == 3:
        cosine = cosine[:, None, :]
        sine = sine[:, None, :]
    first = values[..., :half]
    second = values[..., half:]
    return jnp.concatenate(
        [first * cosine - second * sine, second * cosine + first * sine], axis=-1
    )


def short_conv(values, edge, taps):
    span = taps.shape[0]
    length = values.shape[0]
    padded = jnp.concatenate([edge, values], axis=0).astype(jnp.float32)
    result = jnp.zeros(values.shape, jnp.float32)
    for index in range(span):
        result = result + taps[index].astype(jnp.float32)[None, :] * padded[index : index + length]
    return jax.nn.silu(result).astype(jnp.bfloat16)


def local_scan(heads, steps, decays, writes, reads):
    length = decays.shape[-1]
    running = jnp.einsum(
        "grs,ls->grl",
        decays,
        jnp.tril(jnp.ones((length, length), jnp.float32)),
        precision=lax.Precision.HIGHEST,
    )
    causal = jnp.tril(jnp.ones((length, length), dtype=bool))
    spread = jnp.where(causal, running[..., :, None] - running[..., None, :], -jnp.inf)
    inner = jnp.einsum("gln,gsn->gls", reads, writes, preferred_element_type=jnp.float32)
    mixing = inner[:, None] * jnp.exp(spread) * steps[:, :, None, :]
    within = jnp.einsum(
        "grls,grsp->grlp",
        mixing.astype(jnp.bfloat16),
        heads,
        preferred_element_type=jnp.float32,
    )
    to_end = jnp.exp(running[..., -1:] - running) * steps
    weighted = (heads.astype(jnp.float32) * to_end[..., None]).astype(jnp.bfloat16)
    state = jnp.einsum(
        "grsp,gsn->grpn", weighted, writes, preferred_element_type=jnp.float32
    )
    return running, state, within


def exchange(items, plane, name, number):
    devices, cores = lax.axis_size("sp"), lax.axis_size("tp")
    planes = devices // plane
    counts = [{"plane": plane, "line": planes, "all": devices}[item[1]] for item in items]
    amount = len(items)
    starts = [sum(counts[:i]) for i in range(amount)]
    whole = any(item[1] == "all" for item in items)
    shared = any(item[2] for item in items)

    def kernel(*refs):
        ins, outs = refs[:amount], refs[amount : 2 * amount]
        send, recv, pass_send, pass_recv, own = refs[2 * amount :]
        here, core = lax.axis_index("sp"), lax.axis_index("tp")
        across, within = here // plane, here % plane

        def place(reach, step):
            if reach == "plane":
                slot = (within + step + plane) % plane
                return across * plane + slot, slot
            if reach == "line":
                slot = (across + step + planes) % planes
                return slot * plane + within, slot
            slot = (here + step + devices) % devices
            return slot, slot

        barrier = pltpu.get_barrier_semaphore()
        greeted = 0
        for reach in ("plane", "line", "all"):
            if reach == "all" and not whole or reach != "all" and whole:
                continue
            if not any(item[1] == reach for item in items):
                continue
            size = {"plane": plane, "line": planes, "all": devices}[reach]
            for step in range(1, size):
                pl.semaphore_signal(
                    barrier,
                    inc=1,
                    device_id=(place(reach, step)[0], core),
                    device_id_type=pl.DeviceIdType.MESH,
                )
                greeted += 1
        if shared:
            for turn in range(1, cores):
                pl.semaphore_signal(
                    barrier,
                    inc=1,
                    device_id=(here, (core + turn) % cores),
                    device_id_type=pl.DeviceIdType.MESH,
                )
                greeted += 1
        pl.semaphore_wait(barrier, greeted)

        def target(i, slot, who):
            return outs[i].at[slot, who] if items[i][2] else outs[i].at[slot]

        def sent(i, step):
            goal, goal_slot = place(items[i][1], step)
            mine = place(items[i][1], 0)[1]
            return pltpu.make_async_remote_copy(
                src_ref=ins[i].at[goal_slot] if items[i][3] else ins[i],
                dst_ref=target(i, mine, core),
                send_sem=send.at[starts[i] + step],
                recv_sem=recv.at[starts[i] + step],
                device_id=(goal, core),
                device_id_type=pl.DeviceIdType.MESH,
            )

        def arrived(i, step):
            slot = place(items[i][1], -step)[1]
            return pltpu.make_async_remote_copy(
                src_ref=ins[i].at[slot] if items[i][3] else ins[i],
                dst_ref=target(i, slot, core),
                send_sem=send.at[starts[i] + step],
                recv_sem=recv.at[starts[i] + step],
                device_id=(here, core),
                device_id_type=pl.DeviceIdType.MESH,
            )

        def passed(i, step, turn, outgoing):
            slot = place(items[i][1], -step)[1]
            other = (core + turn) % cores
            owner = core if outgoing else (core - turn + cores) % cores
            return pltpu.make_async_remote_copy(
                src_ref=ins[i] if step == 0 else target(i, slot, core),
                dst_ref=target(i, slot, owner),
                send_sem=pass_send.at[(starts[i] + step) * cores + turn],
                recv_sem=pass_recv.at[(starts[i] + step) * cores + turn],
                device_id=(here, other),
                device_id_type=pl.DeviceIdType.MESH,
            )

        kept = []
        for i in range(amount):
            for step in range(1, counts[i]):
                sent(i, step).start()
        for i in range(amount):
            slot = place(items[i][1], 0)[1]
            local = pltpu.make_async_copy(
                ins[i].at[slot] if items[i][3] else ins[i], target(i, slot, core), own.at[i]
            )
            local.start()
            kept.append(local)
            if items[i][2]:
                for turn in range(1, cores):
                    passed(i, 0, turn, True).start()
        for i in range(amount):
            for step in range(1, counts[i]):
                arrived(i, step).wait_recv()
                if items[i][2]:
                    for turn in range(1, cores):
                        passed(i, step, turn, True).start()
        for i in range(amount):
            kept[i].wait()
            for step in range(counts[i]):
                if step > 0:
                    sent(i, step).wait_send()
                if items[i][2]:
                    for turn in range(1, cores):
                        passed(i, step, turn, True).wait_send()
                        passed(i, step, turn, False).wait_recv()

    shapes = []
    for (array, reach, over, selected), count in zip(items, counts):
        lead = (count, cores) if over else (count,)
        tail = array.shape[1:] if selected else array.shape
        shapes.append(jax.ShapeDtypeStruct(lead + tail, array.dtype))
    slots = sum(counts)
    return pl.pallas_call(
        kernel,
        out_shape=shapes,
        in_specs=[pl.BlockSpec(memory_space=pltpu.VMEM)] * amount,
        out_specs=[pl.BlockSpec(memory_space=pl.ANY)] * amount,
        scratch_shapes=[
            pltpu.SemaphoreType.DMA((slots,)),
            pltpu.SemaphoreType.DMA((slots,)),
            pltpu.SemaphoreType.DMA((slots * cores,)),
            pltpu.SemaphoreType.DMA((slots * cores,)),
            pltpu.SemaphoreType.DMA((amount,)),
        ],
        compiler_params=pltpu.CompilerParams(
            collective_id=number, has_side_effects=True, vmem_limit_bytes=16 * 1024 * 1024
        ),
        cost_estimate=pl.CostEstimate(
            flops=10**8, bytes_accessed=4 * 2**20, transcendentals=0
        ),
        name=name,
    )(*[item[0] for item in items])


def plain_exchange(items, plane):
    results = []
    for array, reach, over, selected in items:
        value = array
        if over:
            value = lax.all_gather(value, "tp")
        if reach == "plane":
            value = value if selected else value[None]
        else:
            value = lax.all_gather(value, "sp")
        results.append(value)
    return results


def gated_norm(mixed, gate, gain):
    length = mixed.shape[0]
    groups = mixed.shape[1]
    flat = mixed.reshape(length, groups, -1)
    gated = flat * jax.nn.silu(gate.astype(jnp.float32)).reshape(length, groups, -1)
    scaled = gated * lax.rsqrt(jnp.mean(gated * gated, axis=-1, keepdims=True) + eps)
    return (scaled * gain.reshape(groups, -1)[None]).reshape(length, -1).astype(jnp.bfloat16)


def attend_piece(
    carry,
    query_plain,
    query_turned,
    query_positions,
    latent,
    key_turned,
    key_positions,
    key_up,
    value_up_weight,
):
    highest, total, summed = carry
    heads = query_plain.shape[1]
    count = latent.shape[0]
    key_plain = (
        jnp.dot(latent, key_up, preferred_element_type=jnp.float32)
        .astype(jnp.bfloat16)
        .reshape(count, heads, -1)
    )
    values = (
        jnp.dot(latent, value_up_weight, preferred_element_type=jnp.float32)
        .astype(jnp.bfloat16)
        .reshape(count, heads, -1)
    )
    scale = (query_plain.shape[-1] + query_turned.shape[-1]) ** (-0.5)
    query_whole = jnp.concatenate([query_plain, query_turned], axis=-1)
    shared_turned = jnp.broadcast_to(key_turned[:, None, :], (count, heads, key_turned.shape[-1]))
    key_whole = jnp.concatenate([key_plain, shared_turned], axis=-1)
    scores = (
        jnp.einsum("qhd,khd->hqk", query_whole, key_whole, preferred_element_type=jnp.float32)
        * scale
    )
    scores = jnp.where(
        key_positions[None, None, :] <= query_positions[None, :, None], scores, -jnp.inf
    )
    new_highest = jnp.maximum(highest, jnp.max(scores, axis=-1))
    weights = jnp.exp(scores - new_highest[..., None])
    total = jnp.sum(weights, axis=-1)
    summed = jnp.einsum(
        "hqk,khd->hqd", weights.astype(jnp.bfloat16), values, preferred_element_type=jnp.float32
    )
    return (new_highest, total, summed)


def shards(
    tokens,
    mix_gain,
    query_proj,
    compressed_projection,
    compressed_norm_gain,
    rope_proj,
    key_up,
    value_up_weight,
    scan_input,
    scan_gate,
    scan_write,
    scan_read,
    step_proj,
    conv_input,
    conv_write,
    conv_read,
    decay_log,
    decay_offset,
    skip_gain,
    group_gain,
):
    groups = scan_write.shape[1] // SSM_STATE
    devices, cores = lax.axis_size("sp"), lax.axis_size("tp")
    plane = groups if devices % groups == 0 else 1
    planes = devices // plane
    sp_index, core = lax.axis_index("sp"), lax.axis_index("tp")
    across, within = sp_index // plane, sp_index % plane
    own_groups = groups // plane
    direct = plane > 1

    def move(items, name, number):
        return exchange(items, plane, name, number) if direct else plain_exchange(items, plane)

    depth = scan_input.shape[0]
    widths = [w.shape[1] // plane for w in (scan_input, scan_gate, scan_write, scan_read)]
    offsets = [sum(widths[:i]) for i in range(4)]
    packed = jnp.stack(
        [
            jnp.concatenate(
                [
                    w[:, n * size : (n + 1) * size]
                    for w, size in zip((scan_input, scan_gate, scan_write, scan_read), widths)
                ],
                axis=1,
            )
            for n in range(plane)
        ]
    )
    (part_weights,) = move([(packed, "plane", False, True)], "weights_in_plane", 1)
    weights = lax.all_gather(
        part_weights.reshape(plane * depth, -1),
        "sp",
        axis=0,
        tiled=True,
        axis_index_groups=[[p * plane + n for p in range(planes)] for n in range(plane)],
    )

    own_normed = rms_scale(tokens, mix_gain).astype(jnp.bfloat16)
    part = tokens.shape[0]
    length = part * cores
    latent_width = compressed_projection.shape[1]
    small = jnp.dot(
        own_normed,
        jnp.concatenate([compressed_projection, rope_proj], axis=1),
        preferred_element_type=jnp.float32,
    )
    latent = rms_scale(small[:, :latent_width], compressed_norm_gain).astype(jnp.bfloat16)
    part_positions = sp_index * length + core * part + jnp.arange(part, dtype=jnp.int32)
    key_turned = rotate(small[:, latent_width:], part_positions).astype(jnp.bfloat16)
    padding = jnp.zeros((part, -(latent_width + ROPE) % 128), jnp.bfloat16)
    own_keys = jnp.concatenate([latent, key_turned, padding], axis=1)
    all_keys, all_rows, offsets_seen = move(
        [
            (own_keys, "all", True, False),
            (own_normed, "plane", True, False),
            (decay_offset.T, "plane", False, False),
        ],
        "rows_and_keys",
        2,
    )
    all_keys = all_keys.reshape(devices * length, -1)
    all_rows = all_rows.reshape(plane * length, -1)
    edge_rows = from_behind(all_rows[plane * length - 8 :], "sp", plane)
    positions = sp_index * length + jnp.arange(length, dtype=jnp.int32)
    rows = lax.dynamic_slice_in_dim(all_rows, within * length, length, 0)
    heads = key_up.shape[1] // UNROTATED_WIDTH

    query = jnp.dot(rows, query_proj, preferred_element_type=jnp.float32).astype(jnp.bfloat16)
    query = query.reshape(length, heads, UNROTATED_WIDTH + ROPE)
    query_plain = query[:, :, :UNROTATED_WIDTH]
    query_turned = rotate(query[:, :, UNROTATED_WIDTH:].astype(jnp.float32), positions).astype(
        jnp.bfloat16
    )
    initial = (
        jnp.full((heads, length), floor_score, jnp.float32),
        jnp.zeros((heads, length), jnp.float32),
        jnp.zeros((heads, length, VALUE_WIDTH), jnp.float32),
    )
    key_positions = jnp.arange(all_keys.shape[0], dtype=jnp.int32)
    _, total, summed = attend_piece(
        initial,
        query_plain,
        query_turned,
        positions,
        all_keys[:, :latent_width],
        all_keys[:, latent_width : latent_width + ROPE],
        key_positions,
        key_up,
        value_up_weight,
    )
    attended = jnp.transpose((summed / total[..., None]).astype(jnp.bfloat16), (1, 0, 2)).reshape(
        length, heads * VALUE_WIDTH
    )

    def own_part(array, axis, size):
        return lax.dynamic_slice_in_dim(array, within * size, size, axis)

    local_heads = decay_log.shape[0]
    own_heads = local_heads // plane
    per_group = local_heads // groups
    step_raw = jnp.dot(
        all_rows,
        lax.dynamic_slice_in_dim(
            step_proj, core * local_heads + within * own_heads, own_heads, 1
        ),
        preferred_element_type=jnp.float32,
    )
    step_size = jax.nn.softplus(step_raw)
    own_offset = own_part(offsets_seen, 1, own_heads)
    step_values = jnp.transpose(step_size.reshape(plane, length, own_heads), (0, 2, 1))
    decay_values = (
        -jnp.exp(own_part(decay_log, 0, own_heads))[None, :, None] * step_values + own_offset
    )

    projected = jnp.dot(all_rows, weights, preferred_element_type=jnp.float32).astype(jnp.bfloat16)
    edge = jnp.dot(edge_rows, weights, preferred_element_type=jnp.float32).astype(jnp.bfloat16)
    span = conv_input.shape[0] - 1

    def convolved(i, taps):
        at = slice(offsets[i], offsets[i] + widths[i])
        return short_conv(projected[:, at], edge[8 - span :, at], own_part(taps, 1, widths[i]))

    head_conv = convolved(0, conv_input)
    gate = projected[:, offsets[1] : offsets[1] + widths[1]]
    writes = convolved(2, conv_write)
    reads = convolved(3, conv_read)
    blocks = plane * own_groups

    def by_block(values, last):
        split = values.reshape(plane, length, own_groups, last)
        return jnp.transpose(split, (0, 2, 1, 3)).reshape(blocks, length, last)

    head_values = jnp.transpose(
        head_conv.reshape(plane, length, own_groups, per_group, SSM_DIM), (0, 2, 3, 1, 4)
    ).reshape(blocks, per_group, length, SSM_DIM)
    write_values = by_block(writes, SSM_STATE)
    read_values = by_block(reads, SSM_STATE)
    running, state, mixed = local_scan(
        head_values,
        step_values.reshape(blocks, per_group, length),
        decay_values.reshape(blocks, per_group, length),
        write_values,
        read_values,
    )
    states = state.reshape(plane, own_heads, SSM_DIM, SSM_STATE)
    totals = running[..., -1].reshape(plane, own_heads)
    before, decayed = [jnp.zeros_like(states[0])], [jnp.zeros_like(totals[0])]
    for index in range(plane):
        before.append(jnp.exp(totals[index])[:, None, None] * before[-1] + states[index])
        decayed.append(totals[index] + decayed[-1])
    sent_total = jnp.pad(decayed[-1][None, :], ((0, 7), (0, 128 - own_heads)))
    seen_states, seen_totals = move(
        [
            (before[-1].reshape(-1, SSM_STATE).astype(jnp.bfloat16), "line", False, False),
            (sent_total, "line", False, False),
        ],
        "states",
        3,
    )
    seen_states = seen_states.reshape(planes, own_heads, SSM_DIM, SSM_STATE).astype(jnp.float32)
    seen_totals = seen_totals[:, 0, :own_heads]
    index = jnp.arange(planes)
    between = (index[None, :] > index[:, None]) & (index[None, :] < across)
    path = jnp.sum(jnp.where(between[:, :, None], seen_totals[None], 0.0), axis=1)
    reached = (index < across)[:, None]
    factor = jnp.where(reached, jnp.exp(path), 0.0)
    incoming = jnp.sum(seen_states * factor[:, :, None, None], axis=0)
    entered = jnp.stack(
        [
            before[k] + jnp.exp(decayed[k])[:, None, None] * incoming
            for k in range(plane)
        ]
    ).reshape(blocks, per_group, SSM_DIM, SSM_STATE)
    carried = jnp.einsum(
        "gln,grpn->grlp",
        read_values,
        entered.astype(jnp.bfloat16),
        preferred_element_type=jnp.float32,
    )
    skip = jnp.broadcast_to(
        own_part(skip_gain, 0, own_heads).reshape(1, own_groups, per_group),
        (plane, own_groups, per_group),
    ).reshape(blocks, per_group, 1, 1)
    mixed = (
        mixed
        + carried * jnp.exp(running)[..., None]
        + skip * head_values.astype(jnp.float32)
    )
    mixed = jnp.transpose(
        mixed.reshape(plane, own_groups, per_group, length, SSM_DIM), (0, 3, 1, 2, 4)
    ).reshape(plane * length, own_groups, per_group, SSM_DIM)
    scanned = gated_norm(mixed, gate, own_part(group_gain, 0, widths[0]))
    (columns,) = move(
        [(scanned.reshape(plane, length, -1), "plane", False, True)], "outputs_in_plane", 4
    )
    scanned = jnp.transpose(columns, (1, 0, 2)).reshape(length, -1)
    return (attended, scanned)


def solution(mesh):
    in_specs = (
        P(("sp", "tp"), None),
        P(),
        P(None, "tp"),
        P(),
        P(),
        P(),
        P(None, "tp"),
        P(None, "tp"),
        P("sp", "tp"),
        P("sp", "tp"),
        P("sp", "tp"),
        P("sp", "tp"),
        P(),
        P(None, "tp"),
        P(None, "tp"),
        P(None, "tp"),
        P("tp"),
        P("sp", "tp"),
        P("tp"),
        P("tp"),
    )
    out_specs = (P("sp", "tp"), P("sp", "tp"))
    return jax.shard_map(shards, mesh=mesh, in_specs=in_specs, out_specs=out_specs, check_vma=False)
```

```python
import jax
import jax.numpy as jnp
from jax import lax
from jax.experimental import pallas as pl
from jax.experimental.pallas import tpu as pltpu
from jax.sharding import PartitionSpec as P

UNROTATED_WIDTH = 128
ROPE = 64
VALUE_WIDTH = 128
SSM_DIM = 64
SSM_STATE = 128


eps = 1e-06
theta = 10000.0
floor_score = -1e30


def from_behind(value, axis, steps):
    count = lax.axis_size(axis)
    initial, last = (max(0, -steps), min(count, count - steps))
    return lax.ppermute(value, axis, [(source, source + steps) for source in range(initial, last)])


def rms_scale(values, gain):
    wide = values.astype(jnp.float32)
    return wide * lax.rsqrt(jnp.mean(wide * wide, axis=-1, keepdims=True) + eps) * gain


def rotate(values, positions):
    half = values.shape[-1] // 2
    freqs = theta ** (-jnp.arange(half, dtype=jnp.float32) * 2.0 / values.shape[-1])
    angle = positions.astype(jnp.float32)[:, None] * freqs[None, :]
    cosine = jnp.cos(angle)
    sine = jnp.sin(angle)
    if values.ndim == 3:
        cosine = cosine[:, None, :]
        sine = sine[:, None, :]
    first = values[..., :half]
    second = values[..., half:]
    return jnp.concatenate(
        [first * cosine - second * sine, second * cosine + first * sine], axis=-1
    )


def short_conv(values, edge, taps):
    span = taps.shape[0]
    length = values.shape[0]
    padded = jnp.concatenate([edge, values], axis=0).astype(jnp.float32)
    result = jnp.zeros(values.shape, jnp.float32)
    for index in range(span):
        result = result + taps[index].astype(jnp.float32)[None, :] * padded[index : index + length]
    return jax.nn.silu(result).astype(jnp.bfloat16)


def local_scan(heads, steps, decays, writes, reads):
    length = decays.shape[-1]
    running = jnp.einsum(
        "grs,ls->grl",
        decays,
        jnp.tril(jnp.ones((length, length), jnp.float32)),
        precision=lax.Precision.HIGHEST,
    )
    causal = jnp.tril(jnp.ones((length, length), dtype=bool))
    spread = jnp.where(causal, running[..., :, None] - running[..., None, :], -jnp.inf)
    inner = jnp.einsum("gln,gsn->gls", reads, writes, preferred_element_type=jnp.float32)
    mixing = inner[:, None] * jnp.exp(spread) * steps[:, :, None, :]
    within = jnp.einsum(
        "grls,grsp->grlp",
        mixing.astype(jnp.bfloat16),
        heads,
        preferred_element_type=jnp.float32,
    )
    to_end = jnp.exp(running[..., -1:] - running) * steps
    weighted = (heads.astype(jnp.float32) * to_end[..., None]).astype(jnp.bfloat16)
    state = jnp.einsum(
        "grsp,gsn->grpn", weighted, writes, preferred_element_type=jnp.float32
    )
    return running, state, within


def exchange(items, plane, name, number):
    devices, cores = lax.axis_size("sp"), lax.axis_size("tp")
    planes = devices // plane
    counts = [{"plane": plane, "line": planes, "all": devices}[item[1]] for item in items]
    amount = len(items)
    starts = [sum(counts[:i]) for i in range(amount)]
    shared = any(item[2] for item in items)

    def kernel(*refs):
        ins, outs = refs[:amount], refs[amount : 2 * amount]
        send, recv, pass_send, pass_recv, own = refs[2 * amount :]
        here, core = lax.axis_index("sp"), lax.axis_index("tp")
        across, within = here // plane, here % plane

        def place(reach, step):
            if reach == "plane":
                slot = (within + step + plane) % plane
                return across * plane + slot, slot
            if reach == "line":
                slot = (across + step + planes) % planes
                return slot * plane + within, slot
            up, along = step // plane, step % plane
            if step < 0:
                up, along = -((-step) // plane), -((-step) % plane)
            slot = (across + up + planes) % planes * plane + (within + along + plane) % plane
            return slot, slot

        barrier = pltpu.get_barrier_semaphore()
        greeted = 0
        for reach in ("plane", "line"):
            if not any(item[1] in (reach, "all") for item in items):
                continue
            size = {"plane": plane, "line": planes}[reach]
            for step in range(1, size):
                pl.semaphore_signal(
                    barrier,
                    inc=1,
                    device_id=(place(reach, step)[0], core),
                    device_id_type=pl.DeviceIdType.MESH,
                )
                greeted += 1
        if shared:
            for turn in range(1, cores):
                pl.semaphore_signal(
                    barrier,
                    inc=1,
                    device_id=(here, (core + turn) % cores),
                    device_id_type=pl.DeviceIdType.MESH,
                )
                greeted += 1
        pl.semaphore_wait(barrier, greeted)

        def target(i, slot, who):
            return outs[i].at[slot, who] if items[i][2] else outs[i].at[slot]

        def sent(i, step):
            goal, goal_slot = place(items[i][1], step)
            mine = place(items[i][1], 0)[1]
            if items[i][1] == "all" and step % plane and step >= plane:
                from_line = place("all", -(step // plane * plane))[1]
                return pltpu.make_async_remote_copy(
                    src_ref=target(i, from_line, core),
                    dst_ref=target(i, from_line, core),
                    send_sem=send.at[starts[i] + step],
                    recv_sem=recv.at[starts[i] + step],
                    device_id=(place("plane", step % plane)[0], core),
                    device_id_type=pl.DeviceIdType.MESH,
                )
            return pltpu.make_async_remote_copy(
                src_ref=ins[i].at[goal_slot] if items[i][3] else ins[i],
                dst_ref=target(i, mine, core),
                send_sem=send.at[starts[i] + step],
                recv_sem=recv.at[starts[i] + step],
                device_id=(goal, core),
                device_id_type=pl.DeviceIdType.MESH,
            )

        def arrived(i, step):
            slot = place(items[i][1], -step)[1]
            return pltpu.make_async_remote_copy(
                src_ref=ins[i].at[slot] if items[i][3] else ins[i],
                dst_ref=target(i, slot, core),
                send_sem=send.at[starts[i] + step],
                recv_sem=recv.at[starts[i] + step],
                device_id=(here, core),
                device_id_type=pl.DeviceIdType.MESH,
            )

        def passed(i, step, turn, outgoing):
            slot = place(items[i][1], -step)[1]
            other = (core + turn) % cores
            owner = core if outgoing else (core - turn + cores) % cores
            return pltpu.make_async_remote_copy(
                src_ref=ins[i] if step == 0 else target(i, slot, core),
                dst_ref=target(i, slot, owner),
                send_sem=pass_send.at[(starts[i] + step) * cores + turn],
                recv_sem=pass_recv.at[(starts[i] + step) * cores + turn],
                device_id=(here, other),
                device_id_type=pl.DeviceIdType.MESH,
            )

        kept = []
        for i in range(amount):
            if items[i][1] == "all":
                for up in range(1, planes):
                    sent(i, up * plane).start()
                for step in range(1, plane):
                    sent(i, step).start()
        for i in range(amount):
            slot = place(items[i][1], 0)[1]
            local = pltpu.make_async_copy(
                ins[i].at[slot] if items[i][3] else ins[i], target(i, slot, core), own.at[i]
            )
            local.start()
            kept.append(local)
            if items[i][2]:
                for turn in range(1, cores):
                    passed(i, 0, turn, True).start()
        for i in range(amount):
            if items[i][1] == "all":
                for up in range(1, planes):
                    arrived(i, up * plane).wait_recv()
                    for step in range(up * plane + 1, (up + 1) * plane):
                        sent(i, step).start()
                    for turn in range(1, cores):
                        passed(i, up * plane, turn, True).start()
        for i in range(amount):
            if items[i][1] != "all":
                for step in range(1, counts[i]):
                    sent(i, step).start()
        for i in range(amount):
            for step in range(1, counts[i]):
                if items[i][1] == "all" and step % plane == 0:
                    continue
                arrived(i, step).wait_recv()
                if items[i][2]:
                    for turn in range(1, cores):
                        passed(i, step, turn, True).start()
        for i in range(amount):
            kept[i].wait()
            for step in range(counts[i]):
                if step > 0:
                    sent(i, step).wait_send()
                if items[i][2]:
                    for turn in range(1, cores):
                        passed(i, step, turn, True).wait_send()
                        passed(i, step, turn, False).wait_recv()

    shapes = []
    for (array, reach, over, selected), count in zip(items, counts):
        lead = (count, cores) if over else (count,)
        tail = array.shape[1:] if selected else array.shape
        shapes.append(jax.ShapeDtypeStruct(lead + tail, array.dtype))
    slots = sum(counts)
    return pl.pallas_call(
        kernel,
        out_shape=shapes,
        in_specs=[pl.BlockSpec(memory_space=pltpu.VMEM)] * amount,
        out_specs=[pl.BlockSpec(memory_space=pl.ANY)] * amount,
        scratch_shapes=[
            pltpu.SemaphoreType.DMA((slots,)),
            pltpu.SemaphoreType.DMA((slots,)),
            pltpu.SemaphoreType.DMA((slots * cores,)),
            pltpu.SemaphoreType.DMA((slots * cores,)),
            pltpu.SemaphoreType.DMA((amount,)),
        ],
        compiler_params=pltpu.CompilerParams(
            collective_id=number, has_side_effects=True, vmem_limit_bytes=16 * 1024 * 1024
        ),
        cost_estimate=pl.CostEstimate(
            flops=10**8, bytes_accessed=4 * 2**20, transcendentals=0
        ),
        name=name,
    )(*[item[0] for item in items])


def plain_exchange(items, plane):
    results = []
    for array, reach, over, selected in items:
        value = array
        if over:
            value = lax.all_gather(value, "tp")
        if reach == "plane":
            value = value if selected else value[None]
        else:
            value = lax.all_gather(value, "sp")
        results.append(value)
    return results


def gated_norm(mixed, gate, gain):
    length = mixed.shape[0]
    groups = mixed.shape[1]
    flat = mixed.reshape(length, groups, -1)
    gated = flat * jax.nn.silu(gate.astype(jnp.float32)).reshape(length, groups, -1)
    scaled = gated * lax.rsqrt(jnp.mean(gated * gated, axis=-1, keepdims=True) + eps)
    return (scaled * gain.reshape(groups, -1)[None]).reshape(length, -1).astype(jnp.bfloat16)


def attend(query, cosine, sine, keys, key_up, value_up_weight, length):
    heads = key_up.shape[1] // UNROTATED_WIDTH
    latent_width = key_up.shape[0]
    whole = UNROTATED_WIDTH + ROPE
    half = ROPE // 2
    step = 2 * length if keys.shape[0] % (2 * length) == 0 else length
    scale = whole ** (-0.5)
    contract = (((1,), (1,)), ((), ()))

    def kernel(q_ref, cos_ref, sin_ref, k_ref, ku_ref, vu_ref, out_ref, q_all, top, total, summed):
        start = lax.axis_index("sp") * length
        for h in range(heads):
            base = h * whole
            turn = q_ref[:, base + UNROTATED_WIDTH : base + whole].astype(jnp.float32)
            first, second = turn[:, :half], turn[:, half:]
            turned = jnp.concatenate(
                [
                    first * cos_ref[...] - second * sin_ref[...],
                    second * cos_ref[...] + first * sin_ref[...],
                ],
                axis=1,
            )
            q_all[h] = jnp.concatenate(
                [q_ref[:, base : base + UNROTATED_WIDTH], turned.astype(jnp.bfloat16)], axis=1
            )
        top[...] = jnp.full(top.shape, floor_score, jnp.float32)
        total[...] = jnp.zeros(total.shape, jnp.float32)
        summed[...] = jnp.zeros(summed.shape, jnp.float32)
        row = start + lax.broadcasted_iota(jnp.int32, (length, step), 0)
        column = lax.broadcasted_iota(jnp.int32, (length, step), 1)

        def visit(j, carry):
            at = pl.ds(pl.multiple_of(j * step, step), step)
            latent = k_ref[at, :latent_width]
            turned = k_ref[at, latent_width : latent_width + ROPE]
            seen = column + j * step <= row
            for h in range(heads):
                col = slice(h * UNROTATED_WIDTH, (h + 1) * UNROTATED_WIDTH)
                val = slice(h * VALUE_WIDTH, (h + 1) * VALUE_WIDTH)
                plain = jnp.dot(
                    latent, ku_ref[:, col], preferred_element_type=jnp.float32
                ).astype(jnp.bfloat16)
                values = jnp.dot(
                    latent, vu_ref[:, val], preferred_element_type=jnp.float32
                ).astype(jnp.bfloat16)
                key = jnp.concatenate([plain, turned], axis=1)
                scores = (
                    lax.dot_general(q_all[h], key, contract, preferred_element_type=jnp.float32)
                    * scale
                )
                scores = jnp.where(seen, scores, -jnp.inf)
                old = top[h][:, :1]
                new = jnp.maximum(old, jnp.max(scores, axis=1, keepdims=True))
                weights = jnp.exp(scores - new)
                shrink = jnp.exp(old - new)
                now = jnp.sum(weights, axis=1, keepdims=True)
                total[h] = total[h] * shrink + now
                summed[h] = summed[h] * shrink + jnp.dot(
                    weights.astype(jnp.bfloat16), values, preferred_element_type=jnp.float32
                )
                top[h] = jnp.broadcast_to(new, top.shape[1:])
            return carry

        lax.fori_loop(0, (start + length + step - 1) // step, visit, 0)
        for h in range(heads):
            out_ref[:, h * VALUE_WIDTH : (h + 1) * VALUE_WIDTH] = (
                summed[h] / total[h][:, :1]
            ).astype(jnp.bfloat16)

    return pl.pallas_call(
        kernel,
        out_shape=jax.ShapeDtypeStruct((length, heads * VALUE_WIDTH), jnp.bfloat16),
        in_specs=[pl.BlockSpec(memory_space=pltpu.VMEM)] * 6,
        out_specs=pl.BlockSpec(memory_space=pltpu.VMEM),
        scratch_shapes=[
            pltpu.VMEM((heads, length, whole), jnp.bfloat16),
            pltpu.VMEM((heads, length, 128), jnp.float32),
            pltpu.VMEM((heads, length, 128), jnp.float32),
            pltpu.VMEM((heads, length, VALUE_WIDTH), jnp.float32),
        ],
        compiler_params=pltpu.CompilerParams(vmem_limit_bytes=40 * 1024 * 1024),
        cost_estimate=pl.CostEstimate(
            flops=4 * 10**10, bytes_accessed=4 * 2**20, transcendentals=0
        ),
        name="attend",
    )(query, cosine, sine, keys, key_up, value_up_weight)


def shards(
    tokens,
    mix_gain,
    query_proj,
    compressed_projection,
    compressed_norm_gain,
    rope_proj,
    key_up,
    value_up_weight,
    scan_input,
    scan_gate,
    scan_write,
    scan_read,
    step_proj,
    conv_input,
    conv_write,
    conv_read,
    decay_log,
    decay_offset,
    skip_gain,
    group_gain,
):
    groups = scan_write.shape[1] // SSM_STATE
    devices, cores = lax.axis_size("sp"), lax.axis_size("tp")
    plane = groups if devices % groups == 0 else 1
    planes = devices // plane
    sp_index, core = lax.axis_index("sp"), lax.axis_index("tp")
    across, within = sp_index // plane, sp_index % plane
    own_groups = groups // plane
    direct = plane > 1

    def move(items, name, number):
        return exchange(items, plane, name, number) if direct else plain_exchange(items, plane)

    depth = scan_input.shape[0]
    widths = [w.shape[1] // plane for w in (scan_input, scan_gate, scan_write, scan_read)]
    offsets = [sum(widths[:i]) for i in range(4)]
    packed = jnp.stack(
        [
            jnp.concatenate(
                [
                    w[:, n * size : (n + 1) * size]
                    for w, size in zip((scan_input, scan_gate, scan_write, scan_read), widths)
                ],
                axis=1,
            )
            for n in range(plane)
        ]
    )
    (part_weights,) = move([(packed, "plane", False, True)], "weights_in_plane", 1)
    weights = lax.all_gather(
        part_weights.reshape(plane * depth, -1),
        "sp",
        axis=0,
        tiled=True,
        axis_index_groups=[[p * plane + n for p in range(planes)] for n in range(plane)],
    )

    own_normed = rms_scale(tokens, mix_gain).astype(jnp.bfloat16)
    part = tokens.shape[0]
    length = part * cores
    latent_width = compressed_projection.shape[1]
    small = jnp.dot(
        own_normed,
        jnp.concatenate([compressed_projection, rope_proj], axis=1),
        preferred_element_type=jnp.float32,
    )
    latent = rms_scale(small[:, :latent_width], compressed_norm_gain).astype(jnp.bfloat16)
    part_positions = sp_index * length + core * part + jnp.arange(part, dtype=jnp.int32)
    key_turned = rotate(small[:, latent_width:], part_positions).astype(jnp.bfloat16)
    padding = jnp.zeros((part, -(latent_width + ROPE) % 128), jnp.bfloat16)
    own_keys = jnp.concatenate([latent, key_turned, padding], axis=1)
    all_keys, all_rows, offsets_seen = move(
        [
            (own_keys, "all", True, False),
            (own_normed, "plane", True, False),
            (decay_offset.T, "plane", False, False),
        ],
        "rows_and_keys",
        2,
    )
    all_keys = all_keys.reshape(devices * length, -1)
    all_rows = all_rows.reshape(plane * length, -1)
    edge_rows = from_behind(all_rows[plane * length - 8 :], "sp", plane)
    positions = sp_index * length + jnp.arange(length, dtype=jnp.int32)
    rows = lax.dynamic_slice_in_dim(all_rows, within * length, length, 0)
    query = jnp.dot(rows, query_proj, preferred_element_type=jnp.float32).astype(jnp.bfloat16)
    half = ROPE // 2
    freqs = theta ** (-jnp.arange(half, dtype=jnp.float32) * 2.0 / ROPE)
    angle = positions.astype(jnp.float32)[:, None] * freqs[None, :]
    attended = attend(
        query, jnp.cos(angle), jnp.sin(angle), all_keys, key_up, value_up_weight, length
    )

    def own_part(array, axis, size):
        return lax.dynamic_slice_in_dim(array, within * size, size, axis)

    local_heads = decay_log.shape[0]
    own_heads = local_heads // plane
    per_group = local_heads // groups
    step_raw = jnp.dot(
        all_rows,
        lax.dynamic_slice_in_dim(
            step_proj, core * local_heads + within * own_heads, own_heads, 1
        ),
        preferred_element_type=jnp.float32,
    )
    step_size = jax.nn.softplus(step_raw)
    own_offset = own_part(offsets_seen, 1, own_heads)
    step_values = jnp.transpose(step_size.reshape(plane, length, own_heads), (0, 2, 1))
    decay_values = (
        -jnp.exp(own_part(decay_log, 0, own_heads))[None, :, None] * step_values + own_offset
    )

    projected = jnp.dot(all_rows, weights, preferred_element_type=jnp.float32).astype(jnp.bfloat16)
    edge = jnp.dot(edge_rows, weights, preferred_element_type=jnp.float32).astype(jnp.bfloat16)
    span = conv_input.shape[0] - 1

    def convolved(i, taps):
        at = slice(offsets[i], offsets[i] + widths[i])
        return short_conv(projected[:, at], edge[8 - span :, at], own_part(taps, 1, widths[i]))

    head_conv = convolved(0, conv_input)
    gate = projected[:, offsets[1] : offsets[1] + widths[1]]
    writes = convolved(2, conv_write)
    reads = convolved(3, conv_read)
    blocks = plane * own_groups

    def by_block(values, last):
        split = values.reshape(plane, length, own_groups, last)
        return jnp.transpose(split, (0, 2, 1, 3)).reshape(blocks, length, last)

    head_values = jnp.transpose(
        head_conv.reshape(plane, length, own_groups, per_group, SSM_DIM), (0, 2, 3, 1, 4)
    ).reshape(blocks, per_group, length, SSM_DIM)
    write_values = by_block(writes, SSM_STATE)
    read_values = by_block(reads, SSM_STATE)
    running, state, mixed = local_scan(
        head_values,
        step_values.reshape(blocks, per_group, length),
        decay_values.reshape(blocks, per_group, length),
        write_values,
        read_values,
    )
    states = state.reshape(plane, own_heads, SSM_DIM, SSM_STATE)
    totals = running[..., -1].reshape(plane, own_heads)
    before, decayed = [jnp.zeros_like(states[0])], [jnp.zeros_like(totals[0])]
    for index in range(plane):
        before.append(jnp.exp(totals[index])[:, None, None] * before[-1] + states[index])
        decayed.append(totals[index] + decayed[-1])
    sent_total = jnp.pad(decayed[-1][None, :], ((0, 7), (0, 128 - own_heads)))
    seen_states, seen_totals = move(
        [
            (before[-1].reshape(-1, SSM_STATE).astype(jnp.bfloat16), "line", False, False),
            (sent_total, "line", False, False),
        ],
        "states",
        3,
    )
    seen_states = seen_states.reshape(planes, own_heads, SSM_DIM, SSM_STATE).astype(jnp.float32)
    seen_totals = seen_totals[:, 0, :own_heads]
    index = jnp.arange(planes)
    between = (index[None, :] > index[:, None]) & (index[None, :] < across)
    path = jnp.sum(jnp.where(between[:, :, None], seen_totals[None], 0.0), axis=1)
    reached = (index < across)[:, None]
    factor = jnp.where(reached, jnp.exp(path), 0.0)
    incoming = jnp.sum(seen_states * factor[:, :, None, None], axis=0)
    entered = jnp.stack(
        [
            before[k] + jnp.exp(decayed[k])[:, None, None] * incoming
            for k in range(plane)
        ]
    ).reshape(blocks, per_group, SSM_DIM, SSM_STATE)
    carried = jnp.einsum(
        "gln,grpn->grlp",
        read_values,
        entered.astype(jnp.bfloat16),
        preferred_element_type=jnp.float32,
    )
    skip = jnp.broadcast_to(
        own_part(skip_gain, 0, own_heads).reshape(1, own_groups, per_group),
        (plane, own_groups, per_group),
    ).reshape(blocks, per_group, 1, 1)
    mixed = (
        mixed
        + carried * jnp.exp(running)[..., None]
        + skip * head_values.astype(jnp.float32)
    )
    mixed = jnp.transpose(
        mixed.reshape(plane, own_groups, per_group, length, SSM_DIM), (0, 3, 1, 2, 4)
    ).reshape(plane * length, own_groups, per_group, SSM_DIM)
    scanned = gated_norm(mixed, gate, own_part(group_gain, 0, widths[0]))
    (columns,) = move(
        [(scanned.reshape(plane, length, -1), "plane", False, True)], "outputs_in_plane", 4
    )
    scanned = jnp.transpose(columns, (1, 0, 2)).reshape(length, -1)
    return (attended, scanned)


def solution(mesh):
    in_specs = (
        P(("sp", "tp"), None),
        P(),
        P(None, "tp"),
        P(),
        P(),
        P(),
        P(None, "tp"),
        P(None, "tp"),
        P("sp", "tp"),
        P("sp", "tp"),
        P("sp", "tp"),
        P("sp", "tp"),
        P(),
        P(None, "tp"),
        P(None, "tp"),
        P(None, "tp"),
        P("tp"),
        P("sp", "tp"),
        P("tp"),
        P("tp"),
    )
    out_specs = (P("sp", "tp"), P("sp", "tp"))
    return jax.shard_map(shards, mesh=mesh, in_specs=in_specs, out_specs=out_specs, check_vma=False)
```

```python
import jax
import jax.numpy as jnp
from jax import lax
from jax.experimental import pallas as pl
from jax.experimental.pallas import tpu as pltpu
from jax.sharding import PartitionSpec as P

UNROTATED_WIDTH = 128
ROPE = 64
VALUE_WIDTH = 128
SSM_DIM = 64
SSM_STATE = 128


eps = 1e-06
theta = 10000.0
floor_score = -1e30


def from_behind(value, axis, steps):
    count = lax.axis_size(axis)
    initial, last = (max(0, -steps), min(count, count - steps))
    return lax.ppermute(value, axis, [(source, source + steps) for source in range(initial, last)])


def rms_scale(values, gain):
    wide = values.astype(jnp.float32)
    return wide * lax.rsqrt(jnp.mean(wide * wide, axis=-1, keepdims=True) + eps) * gain


def rotate(values, positions):
    half = values.shape[-1] // 2
    freqs = theta ** (-jnp.arange(half, dtype=jnp.float32) * 2.0 / values.shape[-1])
    angle = positions.astype(jnp.float32)[:, None] * freqs[None, :]
    cosine = jnp.cos(angle)
    sine = jnp.sin(angle)
    if values.ndim == 3:
        cosine = cosine[:, None, :]
        sine = sine[:, None, :]
    first = values[..., :half]
    second = values[..., half:]
    return jnp.concatenate(
        [first * cosine - second * sine, second * cosine + first * sine], axis=-1
    )


def short_conv(values, edge, taps):
    span = taps.shape[0]
    length = values.shape[0]
    padded = jnp.concatenate([edge, values], axis=0).astype(jnp.float32)
    result = jnp.zeros(values.shape, jnp.float32)
    for index in range(span):
        result = result + taps[index].astype(jnp.float32)[None, :] * padded[index : index + length]
    return jax.nn.silu(result).astype(jnp.bfloat16)


def local_scan(heads, steps, decays, writes, reads):
    length = decays.shape[-1]
    running = jnp.einsum(
        "grs,ls->grl",
        decays,
        jnp.tril(jnp.ones((length, length), jnp.float32)),
        precision=lax.Precision.HIGHEST,
    )
    causal = jnp.tril(jnp.ones((length, length), dtype=bool))
    spread = jnp.where(causal, running[..., :, None] - running[..., None, :], -jnp.inf)
    inner = jnp.einsum("gln,gsn->gls", reads, writes, preferred_element_type=jnp.float32)
    mixing = inner[:, None] * jnp.exp(spread) * steps[:, :, None, :]
    within = jnp.einsum(
        "grls,grsp->grlp",
        mixing.astype(jnp.bfloat16),
        heads,
        preferred_element_type=jnp.float32,
    )
    to_end = jnp.exp(running[..., -1:] - running) * steps
    weighted = (heads.astype(jnp.float32) * to_end[..., None]).astype(jnp.bfloat16)
    state = jnp.einsum(
        "grsp,gsn->grpn", weighted, writes, preferred_element_type=jnp.float32
    )
    return running, state, within


def exchange(items, plane, name, number, columns=False):
    devices, cores = lax.axis_size("sp"), lax.axis_size("tp")
    planes = devices // plane
    counts = [{"plane": plane, "line": planes, "all": devices}[item[1]] for item in items]
    amount = len(items)
    starts = [sum(counts[:i]) for i in range(amount)]
    shared = any(item[2] for item in items)

    def kernel(*refs):
        ins, outs = refs[:amount], refs[amount : 2 * amount]
        send, recv, pass_send, pass_recv, own = refs[2 * amount :]
        here, core = lax.axis_index("sp"), lax.axis_index("tp")
        across, within = here // plane, here % plane

        def place(reach, step):
            if reach == "plane":
                slot = (within + step + plane) % plane
                return across * plane + slot, slot
            if reach == "line":
                slot = (across + step + planes) % planes
                return slot * plane + within, slot
            up, along = step // plane, step % plane
            if step < 0:
                up, along = -((-step) // plane), -((-step) % plane)
            slot = (across + up + planes) % planes * plane + (within + along + plane) % plane
            return slot, slot

        barrier = pltpu.get_barrier_semaphore()
        greeted = 0
        for reach in ("plane", "line"):
            if not any(item[1] in (reach, "all") for item in items):
                continue
            size = {"plane": plane, "line": planes}[reach]
            for step in range(1, size):
                pl.semaphore_signal(
                    barrier,
                    inc=1,
                    device_id=(place(reach, step)[0], core),
                    device_id_type=pl.DeviceIdType.MESH,
                )
                greeted += 1
        if shared:
            for turn in range(1, cores):
                pl.semaphore_signal(
                    barrier,
                    inc=1,
                    device_id=(here, (core + turn) % cores),
                    device_id_type=pl.DeviceIdType.MESH,
                )
                greeted += 1
        pl.semaphore_wait(barrier, greeted)

        def target(i, slot, who):
            if columns:
                size = ins[i].shape[-1]
                return outs[i].at[:, pl.ds(pl.multiple_of(slot * size, size), size)]
            return outs[i].at[slot, who] if items[i][2] else outs[i].at[slot]

        def sent(i, step):
            goal, goal_slot = place(items[i][1], step)
            mine = place(items[i][1], 0)[1]
            if items[i][1] == "all" and step % plane and step >= plane:
                from_line = place("all", -(step // plane * plane))[1]
                return pltpu.make_async_remote_copy(
                    src_ref=target(i, from_line, core),
                    dst_ref=target(i, from_line, core),
                    send_sem=send.at[starts[i] + step],
                    recv_sem=recv.at[starts[i] + step],
                    device_id=(place("plane", step % plane)[0], core),
                    device_id_type=pl.DeviceIdType.MESH,
                )
            return pltpu.make_async_remote_copy(
                src_ref=ins[i].at[goal_slot] if items[i][3] else ins[i],
                dst_ref=target(i, mine, core),
                send_sem=send.at[starts[i] + step],
                recv_sem=recv.at[starts[i] + step],
                device_id=(goal, core),
                device_id_type=pl.DeviceIdType.MESH,
            )

        def arrived(i, step):
            slot = place(items[i][1], -step)[1]
            return pltpu.make_async_remote_copy(
                src_ref=ins[i].at[slot] if items[i][3] else ins[i],
                dst_ref=target(i, slot, core),
                send_sem=send.at[starts[i] + step],
                recv_sem=recv.at[starts[i] + step],
                device_id=(here, core),
                device_id_type=pl.DeviceIdType.MESH,
            )

        def passed(i, step, turn, outgoing):
            slot = place(items[i][1], -step)[1]
            other = (core + turn) % cores
            owner = core if outgoing else (core - turn + cores) % cores
            return pltpu.make_async_remote_copy(
                src_ref=ins[i] if step == 0 else target(i, slot, core),
                dst_ref=target(i, slot, owner),
                send_sem=pass_send.at[(starts[i] + step) * cores + turn],
                recv_sem=pass_recv.at[(starts[i] + step) * cores + turn],
                device_id=(here, other),
                device_id_type=pl.DeviceIdType.MESH,
            )

        kept = []
        for i in range(amount):
            if items[i][1] == "all":
                for up in range(1, planes):
                    sent(i, up * plane).start()
                for step in range(1, plane):
                    sent(i, step).start()
        for i in range(amount):
            if items[i][1] != "all":
                for step in range(1, counts[i]):
                    sent(i, step).start()
        for i in range(amount):
            slot = place(items[i][1], 0)[1]
            local = pltpu.make_async_copy(
                ins[i].at[slot] if items[i][3] else ins[i], target(i, slot, core), own.at[i]
            )
            local.start()
            kept.append(local)
            if items[i][2]:
                for turn in range(1, cores):
                    passed(i, 0, turn, True).start()
        for i in range(amount):
            if items[i][1] == "all":
                for up in range(1, planes):
                    arrived(i, up * plane).wait_recv()
                    for step in range(up * plane + 1, (up + 1) * plane):
                        sent(i, step).start()
                    for turn in range(1, cores):
                        passed(i, up * plane, turn, True).start()
        for i in range(amount):
            for step in range(1, counts[i]):
                if items[i][1] == "all" and step % plane == 0:
                    continue
                arrived(i, step).wait_recv()
                if items[i][2]:
                    for turn in range(1, cores):
                        passed(i, step, turn, True).start()
        for i in range(amount):
            kept[i].wait()
            for step in range(counts[i]):
                if step > 0:
                    sent(i, step).wait_send()
                if items[i][2]:
                    for turn in range(1, cores):
                        passed(i, step, turn, True).wait_send()
                        passed(i, step, turn, False).wait_recv()

    shapes = []
    for (array, reach, over, selected), count in zip(items, counts):
        lead = (count, cores) if over else (count,)
        tail = array.shape[1:] if selected else array.shape
        if columns:
            lead, tail = (), (tail[0], count * tail[1])
        shapes.append(jax.ShapeDtypeStruct(lead + tail, array.dtype))
    slots = sum(counts)
    return pl.pallas_call(
        kernel,
        out_shape=shapes,
        in_specs=[pl.BlockSpec(memory_space=pltpu.VMEM)] * amount,
        out_specs=[pl.BlockSpec(memory_space=pl.ANY)] * amount,
        scratch_shapes=[
            pltpu.SemaphoreType.DMA((slots,)),
            pltpu.SemaphoreType.DMA((slots,)),
            pltpu.SemaphoreType.DMA((slots * cores,)),
            pltpu.SemaphoreType.DMA((slots * cores,)),
            pltpu.SemaphoreType.DMA((amount,)),
        ],
        compiler_params=pltpu.CompilerParams(
            collective_id=number, has_side_effects=True, vmem_limit_bytes=16 * 1024 * 1024
        ),
        cost_estimate=pl.CostEstimate(
            flops=10**8, bytes_accessed=4 * 2**20, transcendentals=0
        ),
        name=name,
    )(*[item[0] for item in items])


def plain_exchange(items, plane):
    results = []
    for array, reach, over, selected in items:
        value = array
        if over:
            value = lax.all_gather(value, "tp")
        if reach == "plane":
            value = value if selected else value[None]
        else:
            value = lax.all_gather(value, "sp")
        results.append(value)
    return results


def gated_norm(mixed, gate, gain):
    length = mixed.shape[0]
    groups = mixed.shape[1]
    flat = mixed.reshape(length, groups, -1)
    gated = flat * jax.nn.silu(gate.astype(jnp.float32)).reshape(length, groups, -1)
    scaled = gated * lax.rsqrt(jnp.mean(gated * gated, axis=-1, keepdims=True) + eps)
    return (scaled * gain.reshape(groups, -1)[None]).reshape(length, -1).astype(jnp.bfloat16)


def attend(query, cosine, sine, keys, key_up, value_up_weight, length):
    heads = key_up.shape[1] // UNROTATED_WIDTH
    latent_width = key_up.shape[0]
    whole = UNROTATED_WIDTH + ROPE
    half = ROPE // 2
    step = 2 * length if keys.shape[0] % (2 * length) == 0 else length
    scale = whole ** (-0.5)
    contract = (((1,), (1,)), ((), ()))

    def kernel(q_ref, cos_ref, sin_ref, k_ref, ku_ref, vu_ref, out_ref, q_all, top, total, summed):
        start = lax.axis_index("sp") * length
        for h in range(heads):
            base = h * whole
            turn = q_ref[:, base + UNROTATED_WIDTH : base + whole].astype(jnp.float32)
            first, second = turn[:, :half], turn[:, half:]
            turned = jnp.concatenate(
                [
                    first * cos_ref[...] - second * sin_ref[...],
                    second * cos_ref[...] + first * sin_ref[...],
                ],
                axis=1,
            )
            q_all[h] = jnp.concatenate(
                [q_ref[:, base : base + UNROTATED_WIDTH], turned.astype(jnp.bfloat16)], axis=1
            )
        top[...] = jnp.full(top.shape, floor_score, jnp.float32)
        total[...] = jnp.zeros(total.shape, jnp.float32)
        summed[...] = jnp.zeros(summed.shape, jnp.float32)
        row = start + lax.broadcasted_iota(jnp.int32, (length, step), 0)
        column = lax.broadcasted_iota(jnp.int32, (length, step), 1)

        def visit(j, carry):
            at = pl.ds(pl.multiple_of(j * step, step), step)
            latent = k_ref[at, :latent_width]
            turned = k_ref[at, latent_width : latent_width + ROPE]
            seen = column + j * step <= row
            plain = jnp.dot(latent, ku_ref[...], preferred_element_type=jnp.float32).astype(
                jnp.bfloat16
            )
            all_values = jnp.dot(latent, vu_ref[...], preferred_element_type=jnp.float32).astype(
                jnp.bfloat16
            )
            for h in range(heads):
                values = all_values[:, h * VALUE_WIDTH : (h + 1) * VALUE_WIDTH]
                key = jnp.concatenate(
                    [plain[:, h * UNROTATED_WIDTH : (h + 1) * UNROTATED_WIDTH], turned], axis=1
                )
                scores = (
                    lax.dot_general(q_all[h], key, contract, preferred_element_type=jnp.float32)
                    * scale
                )
                scores = jnp.where(seen, scores, -jnp.inf)
                old = top[h][:, :1]
                new = jnp.maximum(old, jnp.max(scores, axis=1, keepdims=True))
                weights = jnp.exp(scores - new)
                shrink = jnp.exp(old - new)
                now = jnp.sum(weights, axis=1, keepdims=True)
                total[h] = total[h] * shrink + now
                summed[h] = summed[h] * shrink + jnp.dot(
                    weights.astype(jnp.bfloat16), values, preferred_element_type=jnp.float32
                )
                top[h] = jnp.broadcast_to(new, top.shape[1:])
            return carry

        lax.fori_loop(0, (start + length + step - 1) // step, visit, 0)
        for h in range(heads):
            out_ref[:, h * VALUE_WIDTH : (h + 1) * VALUE_WIDTH] = (
                summed[h] / total[h][:, :1]
            ).astype(jnp.bfloat16)

    return pl.pallas_call(
        kernel,
        out_shape=jax.ShapeDtypeStruct((length, heads * VALUE_WIDTH), jnp.bfloat16),
        in_specs=[pl.BlockSpec(memory_space=pltpu.VMEM)] * 6,
        out_specs=pl.BlockSpec(memory_space=pltpu.VMEM),
        scratch_shapes=[
            pltpu.VMEM((heads, length, whole), jnp.bfloat16),
            pltpu.VMEM((heads, length, 128), jnp.float32),
            pltpu.VMEM((heads, length, 128), jnp.float32),
            pltpu.VMEM((heads, length, VALUE_WIDTH), jnp.float32),
        ],
        compiler_params=pltpu.CompilerParams(vmem_limit_bytes=40 * 1024 * 1024),
        cost_estimate=pl.CostEstimate(
            flops=4 * 10**10, bytes_accessed=4 * 2**20, transcendentals=0
        ),
        name="attend",
    )(query, cosine, sine, keys, key_up, value_up_weight)


def shards(
    tokens,
    mix_gain,
    query_proj,
    compressed_projection,
    compressed_norm_gain,
    rope_proj,
    key_up,
    value_up_weight,
    scan_input,
    scan_gate,
    scan_write,
    scan_read,
    step_proj,
    conv_input,
    conv_write,
    conv_read,
    decay_log,
    decay_offset,
    skip_gain,
    group_gain,
):
    groups = scan_write.shape[1] // SSM_STATE
    devices, cores = lax.axis_size("sp"), lax.axis_size("tp")
    plane = groups if devices % groups == 0 else 1
    planes = devices // plane
    sp_index, core = lax.axis_index("sp"), lax.axis_index("tp")
    across, within = sp_index // plane, sp_index % plane
    own_groups = groups // plane
    direct = plane > 1

    def move(items, name, number, columns=False):
        if direct:
            return exchange(items, plane, name, number, columns)
        return plain_exchange(items, plane)

    depth = scan_input.shape[0]
    widths = [w.shape[1] // plane for w in (scan_input, scan_gate, scan_write, scan_read)]
    offsets = [sum(widths[:i]) for i in range(4)]
    packed = jnp.stack(
        [
            jnp.concatenate(
                [
                    w[:, n * size : (n + 1) * size]
                    for w, size in zip((scan_input, scan_gate, scan_write, scan_read), widths)
                ],
                axis=1,
            )
            for n in range(plane)
        ]
    )
    (part_weights,) = move([(packed, "plane", False, True)], "weights_in_plane", 1)
    weights = lax.all_gather(
        part_weights.reshape(plane * depth, -1),
        "sp",
        axis=0,
        tiled=True,
        axis_index_groups=[[p * plane + n for p in range(planes)] for n in range(plane)],
    )

    own_normed = rms_scale(tokens, mix_gain).astype(jnp.bfloat16)
    part = tokens.shape[0]
    length = part * cores
    latent_width = compressed_projection.shape[1]
    small = jnp.dot(
        own_normed,
        jnp.concatenate([compressed_projection, rope_proj], axis=1),
        preferred_element_type=jnp.float32,
    )
    latent = rms_scale(small[:, :latent_width], compressed_norm_gain).astype(jnp.bfloat16)
    part_positions = sp_index * length + core * part + jnp.arange(part, dtype=jnp.int32)
    key_turned = rotate(small[:, latent_width:], part_positions).astype(jnp.bfloat16)
    padding = jnp.zeros((part, -(latent_width + ROPE) % 128), jnp.bfloat16)
    own_keys = jnp.concatenate([latent, key_turned, padding], axis=1)
    all_keys, all_rows, offsets_seen = move(
        [
            (own_keys, "all", True, False),
            (own_normed, "plane", True, False),
            (decay_offset.T, "plane", False, False),
        ],
        "rows_and_keys",
        2,
    )
    all_keys = all_keys.reshape(devices * length, -1)
    all_rows = all_rows.reshape(plane * length, -1)
    edge_rows = from_behind(all_rows[plane * length - 8 :], "sp", plane)
    positions = sp_index * length + jnp.arange(length, dtype=jnp.int32)
    rows = lax.dynamic_slice_in_dim(all_rows, within * length, length, 0)
    query = jnp.dot(rows, query_proj, preferred_element_type=jnp.float32).astype(jnp.bfloat16)
    half = ROPE // 2
    freqs = theta ** (-jnp.arange(half, dtype=jnp.float32) * 2.0 / ROPE)
    angle = positions.astype(jnp.float32)[:, None] * freqs[None, :]
    attended = attend(
        query, jnp.cos(angle), jnp.sin(angle), all_keys, key_up, value_up_weight, length
    )

    def own_part(array, axis, size):
        return lax.dynamic_slice_in_dim(array, within * size, size, axis)

    local_heads = decay_log.shape[0]
    own_heads = local_heads // plane
    per_group = local_heads // groups
    step_raw = jnp.dot(
        all_rows,
        lax.dynamic_slice_in_dim(
            step_proj, core * local_heads + within * own_heads, own_heads, 1
        ),
        preferred_element_type=jnp.float32,
    )
    step_size = jax.nn.softplus(step_raw)
    own_offset = own_part(offsets_seen, 1, own_heads)
    step_values = jnp.transpose(step_size.reshape(plane, length, own_heads), (0, 2, 1))
    decay_values = (
        -jnp.exp(own_part(decay_log, 0, own_heads))[None, :, None] * step_values + own_offset
    )

    projected = jnp.dot(all_rows, weights, preferred_element_type=jnp.float32).astype(jnp.bfloat16)
    edge = jnp.dot(edge_rows, weights, preferred_element_type=jnp.float32).astype(jnp.bfloat16)
    span = conv_input.shape[0] - 1

    def convolved(i, taps):
        at = slice(offsets[i], offsets[i] + widths[i])
        return short_conv(projected[:, at], edge[8 - span :, at], own_part(taps, 1, widths[i]))

    head_conv = convolved(0, conv_input)
    gate = projected[:, offsets[1] : offsets[1] + widths[1]]
    writes = convolved(2, conv_write)
    reads = convolved(3, conv_read)
    blocks = plane * own_groups

    def by_block(values, last):
        split = values.reshape(plane, length, own_groups, last)
        return jnp.transpose(split, (0, 2, 1, 3)).reshape(blocks, length, last)

    head_values = jnp.transpose(
        head_conv.reshape(plane, length, own_groups, per_group, SSM_DIM), (0, 2, 3, 1, 4)
    ).reshape(blocks, per_group, length, SSM_DIM)
    write_values = by_block(writes, SSM_STATE)
    read_values = by_block(reads, SSM_STATE)
    running, state, mixed = local_scan(
        head_values,
        step_values.reshape(blocks, per_group, length),
        decay_values.reshape(blocks, per_group, length),
        write_values,
        read_values,
    )
    states = state.reshape(plane, own_heads, SSM_DIM, SSM_STATE)
    totals = running[..., -1].reshape(plane, own_heads)
    before, decayed = [jnp.zeros_like(states[0])], [jnp.zeros_like(totals[0])]
    for index in range(plane):
        before.append(jnp.exp(totals[index])[:, None, None] * before[-1] + states[index])
        decayed.append(totals[index] + decayed[-1])
    sent_total = jnp.pad(decayed[-1][None, :], ((0, 7), (0, 128 - own_heads)))
    seen_states, seen_totals = move(
        [
            (before[-1].reshape(-1, SSM_STATE).astype(jnp.bfloat16), "line", False, False),
            (sent_total, "line", False, False),
        ],
        "states",
        3,
    )
    seen_states = seen_states.reshape(planes, own_heads, SSM_DIM, SSM_STATE).astype(jnp.float32)
    seen_totals = seen_totals[:, 0, :own_heads]
    index = jnp.arange(planes)
    between = (index[None, :] > index[:, None]) & (index[None, :] < across)
    path = jnp.sum(jnp.where(between[:, :, None], seen_totals[None], 0.0), axis=1)
    reached = (index < across)[:, None]
    factor = jnp.where(reached, jnp.exp(path), 0.0)
    incoming = jnp.sum(seen_states * factor[:, :, None, None], axis=0)
    entered = jnp.stack(
        [
            before[k] + jnp.exp(decayed[k])[:, None, None] * incoming
            for k in range(plane)
        ]
    ).reshape(blocks, per_group, SSM_DIM, SSM_STATE)
    carried = jnp.einsum(
        "gln,grpn->grlp",
        read_values,
        entered.astype(jnp.bfloat16),
        preferred_element_type=jnp.float32,
    )
    skip = jnp.broadcast_to(
        own_part(skip_gain, 0, own_heads).reshape(1, own_groups, per_group),
        (plane, own_groups, per_group),
    ).reshape(blocks, per_group, 1, 1)
    mixed = (
        mixed
        + carried * jnp.exp(running)[..., None]
        + skip * head_values.astype(jnp.float32)
    )
    mixed = jnp.transpose(
        mixed.reshape(plane, own_groups, per_group, length, SSM_DIM), (0, 3, 1, 2, 4)
    ).reshape(plane * length, own_groups, per_group, SSM_DIM)
    scanned = gated_norm(mixed, gate, own_part(group_gain, 0, widths[0]))
    (columns,) = move(
        [(scanned.reshape(plane, length, -1), "plane", False, True)], "outputs_in_plane", 4, True
    )
    scanned = columns.reshape(length, -1)
    return (attended, scanned)


def solution(mesh):
    in_specs = (
        P(("sp", "tp"), None),
        P(),
        P(None, "tp"),
        P(),
        P(),
        P(),
        P(None, "tp"),
        P(None, "tp"),
        P("sp", "tp"),
        P("sp", "tp"),
        P("sp", "tp"),
        P("sp", "tp"),
        P(),
        P(None, "tp"),
        P(None, "tp"),
        P(None, "tp"),
        P("tp"),
        P("sp", "tp"),
        P("tp"),
        P("tp"),
    )
    out_specs = (P("sp", "tp"), P("sp", "tp"))
    return jax.shard_map(shards, mesh=mesh, in_specs=in_specs, out_specs=out_specs, check_vma=False)
```
